32 devices in a mesh: fs: 8 (over z, y), tp: 4 (over x, core).
Axes of the slice: x: 2, y: 2, z: 4, core: 2. Of those that a mesh axis runs over, the one named last changes fastest.
Arguments:
- inputs: bfloat16 [4096, 2304], P('fs'), may hold values from -6 to 6
- value_cot: bfloat16 [4096, 4096], P('fs', 'tp'), may hold values from -0.09375 to 0.09375
- retained: bfloat16 [4096, 4096], P('fs', 'tp'), may hold values from -6 to 6
- output_cot: bfloat16 [4096, 2304], P('fs'), may hold values from -0.09375 to 0.09375
- proj_value: bfloat16 [2304, 192], P('fs'), may hold values from -0.125 to 0.125
- proj_output: bfloat16 [2304, 192], P('fs'), may hold values from -0.125 to 0.125
- w_value: float32 [2304, 4096], P('fs', 'tp'), may hold values from -6 to 6
- w_output: float32 [4096, 2304], P('tp', 'fs'), may hold values from -6 to 6
- first_value: float32 [192, 4096], P('fs', 'tp'), may hold values from -106 to 106
- second_value: float32 [192, 4096], P('fs', 'tp'), may hold values from 0.25 to 4
- first_output: float32 [192, 4096], P('fs', 'tp'), may hold values from -106 to 106
- second_output: float32 [192, 4096], P('fs', 'tp'), may hold values from 0.25 to 4
Outputs:
- step_value: float32 [2304, 4096], P('fs', 'tp')
- step_output: float32 [4096, 2304], P('tp', 'fs')
- copy_value: bfloat16 [2304, 4096], P(None, 'tp')
- copy_output: bfloat16 [4096, 2304], P('tp')
- new_first_value: float32 [192, 4096], P('fs', 'tp')
- new_second_value: float32 [192, 4096], P('fs', 'tp')
- new_first_output: float32 [192, 4096], P('fs', 'tp')
- new_second_output: float32 [192, 4096], P('fs', 'tp')
The draws below stay inside these ranges and needn't reach their ends.
All inputs are finite; a program needn't handle non-finite values.
Results may differ from the reference program's by a relative error of at most 0.0034.
Values may be sent and summed in bfloat16 or wider, within the bound.
A program may use at most 64 MiB of HBM per device.

```python
import math
import jax
import jax.numpy as jnp
from jax import lax

D = 2304
RANK = 192
HV = 4096
TOKENS = 4096


def moment_law(key, row_total, col_total):
    row_pos = jnp.arange(row_total, dtype=jnp.float32) / row_total
    col_pos = jnp.arange(col_total, dtype=jnp.float32) / col_total
    drawn = jnp.clip(jax.random.normal(key, (row_total, col_total), jnp.float32), -6.0, 6.0)
    row_scale = 3.0 ** row_pos
    col_scale = 3.0 ** col_pos
    return drawn * row_scale[:, None] * col_scale[None, :]


def draw_first_value(key, part):
    return moment_law(jax.random.fold_in(key, 11), RANK, HV)


def draw_first_output(key, part):
    return moment_law(jax.random.fold_in(key, 23), RANK, HV)


def block_scale(own_key, dims, shards, least, largest):
    gain, own = 1.0, jax.random.fold_in(own_key, 6)
    for dim, parts in shards:
        steps = jnp.exp(jax.random.uniform(jax.random.fold_in(own, dim), (parts,), jnp.float32, least / len(shards), largest / len(shards)))
        gain = gain * jnp.repeat(steps, dims[dim] // parts).reshape([-1 if axis == dim else 1 for axis in range(len(dims))])
    return gain


def scatter_about(rng, shape, spread, most, shards=(), kind=jnp.bfloat16):
    values = jax.random.normal(rng, shape, jnp.float32) * spread
    if len(shards) > 0:
        values = block_scale(rng, shape, shards, -0.22, 0.18) * values
    return jnp.clip(values, min=-most, max=most).astype(kind)


def setup_inputs(seed: int = 0) -> dict:
    seeds = jax.random.split(jax.random.key(seed), 13)
    inputs = scatter_about(seeds[0], (TOKENS, D), 1.0, 6.0, ((0, 8),))
    value_cot = scatter_about(seeds[1], (TOKENS, HV), (TOKENS ** -0.5), 0.09375, ((0, 8), (1, 4)))
    retained = scatter_about(seeds[2], (TOKENS, HV), 1.0, 6.0, ((0, 8), (1, 4)))
    output_cot = scatter_about(seeds[3], (TOKENS, D), (TOKENS ** -0.5), 0.09375, ((0, 8),))
    proj_value = scatter_about(seeds[4], (D, RANK), D ** -0.5, 0.125, ((0, 8),))
    proj_output = scatter_about(seeds[5], (D, RANK), D ** -0.5, 0.125, ((0, 8),))
    w_value = scatter_about(seeds[6], (D, HV), 1.0, 6.0, ((0, 8), (1, 4)), jnp.float32)
    w_output = scatter_about(seeds[7], (HV, D), 1.0, 6.0, ((0, 4), (1, 8)), jnp.float32)
    first_value = draw_first_value(jax.random.fold_in(seeds[12], 71), 0)
    second_value = jnp.clip(jnp.exp(math.log(4.0) - 2.7725887 * jax.random.uniform(seeds[9], (RANK, HV), jnp.float32) ** block_scale(seeds[9], (RANK, HV), ((0, 8), (1, 4)), -0.2, 0.2)), 0.25, 4.0)
    first_output = draw_first_output(jax.random.fold_in(seeds[12], 71), 0)
    second_output = jnp.clip(jnp.exp(math.log(4.0) - 2.7725887 * jax.random.uniform(seeds[11], (RANK, HV), jnp.float32) ** block_scale(seeds[11], (RANK, HV), ((0, 8), (1, 4)), -0.2, 0.2)), 0.25, 4.0)
    return dict(inputs=inputs, value_cot=value_cot, retained=retained, output_cot=output_cot, proj_value=proj_value, proj_output=proj_output, w_value=w_value, w_output=w_output, first_value=first_value, second_value=second_value, first_output=first_output, second_output=second_output)


beta_one = 0.8
beta_two = 0.9
moment_eps = 1e-08
norm_eps = 1e-06

def adapt(first, second, grad):
    new_first = beta_one * first + (1.0 - beta_one) * grad
    new_second = beta_two * second + (1.0 - beta_two) * grad * grad
    direction = (new_first / (jnp.sqrt(new_second) + moment_eps)).astype(jnp.bfloat16)
    return (new_first, new_second, direction)

def reference(inputs, value_cot, retained, output_cot, proj_value, proj_output, w_value, w_output, first_value, second_value, first_output, second_output):
    x_proj = jnp.dot(inputs, proj_value, preferred_element_type=jnp.float32).astype(jnp.bfloat16)
    o_proj = jnp.dot(output_cot, proj_output, preferred_element_type=jnp.float32).astype(jnp.bfloat16)
    grad_value = jnp.dot(x_proj.T, value_cot, preferred_element_type=jnp.float32)
    grad_output = jnp.dot(o_proj.T, retained, preferred_element_type=jnp.float32)
    first_v, second_v, dir_value = adapt(first_value, second_value, grad_value)
    first_o, second_o, dir_output = adapt(first_output, second_output, grad_output)
    square_v = jnp.sum(jnp.square(dir_value.astype(jnp.float32)))
    square_o = jnp.sum(jnp.square(dir_output.astype(jnp.float32)))
    scale_value = lax.rsqrt(square_v / (RANK * HV) + norm_eps)
    scale_output = lax.rsqrt(square_o / (RANK * HV) + norm_eps)
    step_value = jnp.dot(proj_value, dir_value, preferred_element_type=jnp.float32) * scale_value
    step_output = jnp.dot(dir_output.T, proj_output.T, preferred_element_type=jnp.float32) * scale_output
    copy_value = (w_value + step_value).astype(jnp.bfloat16)
    copy_output = (w_output + step_output).astype(jnp.bfloat16)
    return (step_value, step_output, copy_value, copy_output, first_v, second_v, first_o, second_o)
```

```python
import functools

import jax
import jax.numpy as jnp
from jax import lax
from jax.experimental import pallas as pl
from jax.experimental.pallas import tpu as pltpu
from jax.sharding import PartitionSpec as P

BF16 = jnp.bfloat16
F32 = jnp.float32

beta_one = 0.8
beta_two = 0.9
moment_eps = 1e-08
norm_eps = 1e-06

EARLY_NUM, EARLY_DEN = 1, 2


def adapt(first, second, grad):
    new_first = beta_one * first + (1.0 - beta_one) * grad
    new_second = beta_two * second + (1.0 - beta_two) * grad * grad
    direction = (new_first / (jnp.sqrt(new_second) + moment_eps)).astype(BF16)
    return (new_first, new_second, direction)


def flat(block):
    parts, rows, columns = block.shape
    if rows % 16 == 0:
        return block.reshape(parts * rows, columns)
    return block.astype(F32).reshape(parts * rows, columns).astype(block.dtype)


def exchange(
    n, t, x_ref, oc_ref, vc_ref, ret_ref, pv_ref, po_ref, wv_ref, wo_ref, fv_ref, sv_ref, fo_ref, so_ref,
    wall, pall, dall, sq, nfv, nsv, nfo, nso,
    xin, pr, gsend, grecv,
    load_sem, p_send, p_recv, core_send, core_recv, g_send, g_recv, d_send, d_recv, q_send, q_recv,
    ring_send, ring_recv, y_send, y_recv,
):
    me = lax.axis_index("fs")
    tp = lax.axis_index("tp")
    core = lax.rem(tp, 2)
    partner = tp + 1 - 2 * core
    z, y = me // 2, lax.rem(me, 2)
    levels = n // 2
    across = me + 1 - 2 * y
    q, columns = wv_ref.shape
    rows = 2 * q
    early = max(16, (rows * EARLY_NUM // EARLY_DEN) // 16 * 16)
    late = rows - early
    last = levels // 2
    halved = levels % 2 == 0
    rr = fv_ref.shape[0]

    def remote(src, dst, ssem, rsem, device):
        return pltpu.make_async_remote_copy(
            src_ref=src, dst_ref=dst, send_sem=ssem, recv_sem=rsem,
            device_id=device, device_id_type=pl.DeviceIdType.MESH,
        )

    barrier = pltpu.get_barrier_semaphore()
    for d in range(1, n):
        pl.semaphore_signal(
            barrier, inc=1, device_id={"fs": lax.rem(me + d, n)}, device_id_type=pl.DeviceIdType.MESH
        )
    for d in range(1, t):
        pl.semaphore_signal(
            barrier, inc=1, device_id={"tp": lax.rem(tp + d, t)}, device_id_type=pl.DeviceIdType.MESH
        )

    @pl.when(core == 0)
    def _():
        pltpu.make_async_copy(x_ref, xin, load_sem).start()
        pall[0, me] = pv_ref[...]

    @pl.when(core == 1)
    def _():
        pltpu.make_async_copy(oc_ref, xin, load_sem).start()
        pall[1, me] = po_ref[...]

    wall[me, :q] = wv_ref[...].astype(BF16)
    wall[me, q:] = wo_ref[...].astype(BF16)
    pl.semaphore_wait(barrier, n - 1 + t - 1)

    sends = []

    def go(copy):
        copy.start()
        sends.append(copy)
        return copy

    def to_all(buffer, target, ssem, rsem):
        out = []
        for d in range(1, n):
            peer = lax.rem(me + d, n)
            out.append(go(remote(buffer(peer), target, ssem.at[d], rsem.at[d], {"fs": peer})))
        return out

    def span(piece, k, s):
        low, high = (0, late) if piece == 0 else (late, rows)
        if halved and k == last:
            middle = low + (high - low) // 2 // 16 * 16
            low, high = (low, middle) if s == 0 else (middle, high)
        return low, high - low

    def at(level, column, low, size):
        return wall.at[level * 2 + column, pl.ds(low, size)]

    def ring(piece, k, s):
        low, size = span(piece, k, s)
        if size == 0:
            return None
        step = 1 if s == 0 else levels - 1
        level = lax.rem(z + (levels - step) * (k - 1), levels)
        column = y if piece < 2 else 1 - y
        place = at(level, column, low, size)
        target = lax.rem(z + step, levels) * 2 + y
        return go(remote(place, place, ring_send.at[s, k, piece], ring_recv.at[s, k, piece], {"fs": target}))

    def over(k, s):
        low, size = span(0, k, s)
        if size == 0:
            return None
        step = 1 if s == 0 else levels - 1
        level = lax.rem(z + (levels - step) * k, levels)
        place = at(level, y, low, size)
        return go(remote(place, place, y_send.at[s, k], y_recv.at[s, k], {"fs": across}))

    def landed(copy):
        if copy is not None:
            copy.wait_recv()

    proj_copies = to_all(lambda peer: pall.at[core, me], pall.at[core, me], p_send, p_recv)
    own_early = at(z, y, late, early)
    crossed = go(remote(own_early, own_early, y_send.at[1, 0], y_recv.at[1, 0], {"fs": across}))
    steps = {}
    for piece in (0, 1):
        for s in (0, 1):
            steps[piece, 1, s] = ring(piece, 1, s)
    own_late = at(z, y, 0, late)
    overs = [go(remote(own_late, own_late, y_send.at[0, 0], y_recv.at[0, 0], {"fs": across}))]

    for copy in proj_copies:
        copy.wait_recv()
    whole_proj = go(remote(pall.at[core], pall.at[core], core_send.at[0], core_recv.at[0], {"tp": partner}))
    pltpu.make_async_copy(x_ref, xin, load_sem).wait()
    pr[core] = jnp.dot(xin[...], flat(pall[core]), preferred_element_type=F32).astype(BF16)
    swapped = go(remote(pr.at[core], pr.at[core], core_send.at[1], core_recv.at[1], {"tp": partner}))
    swapped.wait_recv()
    for side, cot in ((0, vc_ref), (1, ret_ref)):
        grad = lax.dot_general(
            pr[side], cot[...], (((0,), (0,)), ((), ())), preferred_element_type=F32
        )
        for peer in range(n):
            gsend[peer, :, side * columns:(side + 1) * columns] = (
                grad[peer * rr:(peer + 1) * rr].astype(BF16)
            )
    grad_copies = to_all(lambda peer: gsend.at[peer], grecv.at[me], g_send, g_recv)

    crossed.wait_recv()
    for s in (0, 1):
        steps[2, 1, s] = ring(2, 1, s)

    dir_copies = []
    for k in range(1, last + 1):
        for piece in (0, 1, 2):
            if k == 1 and piece == 2:
                for copy in grad_copies:
                    copy.wait_recv()
                total = gsend[me].astype(F32)
                for d in range(1, n):
                    total += grecv[lax.rem(me + d, n)].astype(F32)
                for side, refs in ((0, (fv_ref, sv_ref, nfv, nsv)), (1, (fo_ref, so_ref, nfo, nso))):
                    part = total[:, side * columns:(side + 1) * columns]
                    new_first, new_second, direction = adapt(refs[0][...], refs[1][...], part)
                    refs[2][...] = new_first
                    refs[3][...] = new_second
                    dall[me, :, side * columns:(side + 1) * columns] = direction
                dir_copies = to_all(lambda peer: dall.at[me], dall.at[me], d_send, d_recv)
            for s in (0, 1):
                landed(steps[piece, k, s])
                if k < last:
                    steps[piece, k + 1, s] = ring(piece, k + 1, s)
                if piece == 0:
                    overs.append(over(k, s))

    for copy in dir_copies:
        copy.wait_recv()
    sums = []
    for side in (0, 1):
        acc = jnp.zeros((rr, columns), F32)
        for k in range(n):
            acc += jnp.square(dall[k, :, side * columns:(side + 1) * columns].astype(F32))
        sums.append(jnp.sum(acc))
    line = lax.broadcasted_iota(jnp.int32, sq.shape[1:], 0)
    sq[tp] = jnp.where(line == 0, sums[0], sums[1])
    sq_copies = []
    for d in range(1, t):
        sq_copies.append(
            go(remote(sq.at[tp], sq.at[tp], q_send.at[d], q_recv.at[d], {"tp": lax.rem(tp + d, t)}))
        )
    for copy in sq_copies:
        copy.wait_recv()
    for copy in overs:
        landed(copy)
    whole_proj.wait_recv()
    for copy in sends:
        copy.wait_send()


def finish(q, count, sq_ref, wall_ref, pall_ref, own_v, own_o, dv_ref, do_ref, step_v, step_o, copy_v, copy_o):
    totals = jnp.sum(sq_ref[...], axis=0)
    scale_v = lax.rsqrt(totals[0:1, 0:1] / count + norm_eps)
    scale_o = lax.rsqrt(totals[1:2, 0:1] / count + norm_eps)
    n, _, lanes = wall_ref.shape
    dir_v, dir_o = dv_ref[...], do_ref[...]
    step_v[...] = jnp.dot(own_v[...], dir_v, preferred_element_type=F32) * scale_v
    step_o[...] = jnp.dot(own_o[...], dir_o, preferred_element_type=F32) * scale_o
    w_v = wall_ref[:, :q].astype(F32).reshape(n * q, lanes)
    w_o = wall_ref[:, q:].astype(F32).reshape(n * q, lanes)
    copy_v[...] = (
        w_v + jnp.dot(pall_ref[0], dir_v, preferred_element_type=F32) * scale_v
    ).astype(BF16)
    moved = w_o + jnp.dot(pall_ref[1], dir_o, preferred_element_type=F32) * scale_o
    copy_o[...] = moved.T.astype(BF16)


def per_device(
    n, t,
    inputs, value_cot, retained, output_cot, proj_value, proj_output, w_value, w_output,
    first_value, second_value, first_output, second_output,
):
    tokens, width = inputs.shape
    q, rank = proj_value.shape
    columns = value_cot.shape[1]
    rr = first_value.shape[0]
    last = n // 2 // 2
    vmem = pl.BlockSpec(memory_space=pltpu.VMEM)
    anywhere = pl.BlockSpec(memory_space=pl.ANY)
    dma = pltpu.SemaphoreType.DMA
    moment = jax.ShapeDtypeStruct((rr, columns), F32)
    wall, pall, dall, sq, first_v, second_v, first_o, second_o = pl.pallas_call(
        functools.partial(exchange, n, t),
        out_shape=(
            jax.ShapeDtypeStruct((n, 2 * q, columns), BF16),
            jax.ShapeDtypeStruct((2, n, q, rank), BF16),
            jax.ShapeDtypeStruct((n, rr, 2 * columns), BF16),
            jax.ShapeDtypeStruct((t, 8, 128), F32),
            moment, moment, moment, moment,
        ),
        in_specs=[anywhere, anywhere] + [vmem] * 10,
        out_specs=(vmem,) * 8,
        scratch_shapes=[
            pltpu.VMEM((tokens, width), BF16),
            pltpu.VMEM((2, tokens, rank), BF16),
            pltpu.VMEM((n, rr, 2 * columns), BF16),
            pltpu.VMEM((n, rr, 2 * columns), BF16),
            dma, dma((n,)), dma((n,)), dma((2,)), dma((2,)), dma((n,)), dma((n,)), dma((n,)), dma((n,)),
            dma((t,)), dma((t,)),
            dma((2, last + 1, 3)), dma((2, last + 1, 3)), dma((2, last + 1)), dma((2, last + 1)),
        ],
        compiler_params=pltpu.CompilerParams(
            collective_id=0, has_side_effects=True, vmem_limit_bytes=60 * 1024 * 1024
        ),
        name="exchange",
    )(
        inputs, output_cot, value_cot, retained, proj_value, proj_output, w_value, w_output.T,
        first_value, second_value, first_output, second_output,
    )
    lanes = 128
    tiles = columns // lanes
    dirs = dall.reshape(n * rr, 2 * columns)
    full = n * q
    step_v, step_o, copy_v, copy_o = pl.pallas_call(
        functools.partial(finish, q, float(rank * columns * t)),
        grid=(tiles,),
        out_shape=(
            jax.ShapeDtypeStruct((q, columns), F32),
            jax.ShapeDtypeStruct((q, columns), F32),
            jax.ShapeDtypeStruct((full, columns), BF16),
            jax.ShapeDtypeStruct((columns, full), BF16),
        ),
        in_specs=[
            pl.BlockSpec((t, 8, 128), lambda j: (0, 0, 0)),
            pl.BlockSpec((n, 2 * q, lanes), lambda j: (0, 0, j)),
            pl.BlockSpec((2, full, rank), lambda j: (0, 0, 0)),
            pl.BlockSpec((q, rank), lambda j: (0, 0)),
            pl.BlockSpec((q, rank), lambda j: (0, 0)),
            pl.BlockSpec((rank, lanes), lambda j: (0, j)),
            pl.BlockSpec((rank, lanes), lambda j: (0, j + tiles)),
        ],
        out_specs=(
            pl.BlockSpec((q, lanes), lambda j: (0, j)),
            pl.BlockSpec((q, lanes), lambda j: (0, j)),
            pl.BlockSpec((full, lanes), lambda j: (0, j)),
            pl.BlockSpec((lanes, full), lambda j: (j, 0)),
        ),
        compiler_params=pltpu.CompilerParams(vmem_limit_bytes=48 * 1024 * 1024),
        name="finish",
    )(sq, wall, pall.reshape(2, full, rank), proj_value, proj_output, dirs, dirs)
    return (step_v, step_o.T, copy_v, copy_o, first_v, second_v, first_o, second_o)


def solution(mesh):
    in_specs = (
        P("fs", None),
        P("fs", "tp"),
        P("fs", "tp"),
        P("fs", None),
        P("fs", None),
        P("fs", None),
        P("fs", "tp"),
        P("tp", "fs"),
        P("fs", "tp"),
        P("fs", "tp"),
        P("fs", "tp"),
        P("fs", "tp"),
    )
    out_specs = (
        P("fs", "tp"),
        P("tp", "fs"),
        P(None, "tp"),
        P("tp", None),
        P("fs", "tp"),
        P("fs", "tp"),
        P("fs", "tp"),
        P("fs", "tp"),
    )
    return jax.shard_map(
        functools.partial(per_device, mesh.shape["fs"], mesh.shape["tp"]),
        mesh=mesh, in_specs=in_specs, out_specs=out_specs, check_vma=False,
    )
```

```python
import functools

import jax
import jax.numpy as jnp
from jax import lax
from jax.experimental import pallas as pl
from jax.experimental.pallas import tpu as pltpu
from jax.sharding import PartitionSpec as P

BF16 = jnp.bfloat16
F32 = jnp.float32

beta_one = 0.8
beta_two = 0.9
moment_eps = 1e-08
norm_eps = 1e-06

EARLY_NUM, EARLY_DEN = 1, 6
CHUNKS = 4


def adapt(first, second, grad):
    new_first = beta_one * first + (1.0 - beta_one) * grad
    new_second = beta_two * second + (1.0 - beta_two) * grad * grad
    direction = (new_first / (jnp.sqrt(new_second) + moment_eps)).astype(BF16)
    return (new_first, new_second, direction)


def flat(block):
    parts, rows, columns = block.shape
    if rows % 16 == 0:
        return block.reshape(parts * rows, columns)
    return block.astype(F32).reshape(parts * rows, columns).astype(block.dtype)


def exchange(
    n, t, x_ref, oc_ref, vc_ref, ret_ref, pv_ref, po_ref, wv_ref, wo_ref, fv_ref, sv_ref, fo_ref, so_ref,
    wall, pall, dall, sq, nfv, nsv, nfo, nso,
    xin, pr, gsend, grecv,
    load_sem, p_send, p_recv, core_send, core_recv, g_send, g_recv, d_send, d_recv, q_send, q_recv,
    ring_send, ring_recv, y_send, y_recv,
):
    me = lax.axis_index("fs")
    tp = lax.axis_index("tp")
    core = lax.rem(tp, 2)
    partner = tp + 1 - 2 * core
    z, y = me // 2, lax.rem(me, 2)
    levels = n // 2
    across = me + 1 - 2 * y
    q, columns = wv_ref.shape
    rows = 2 * q
    early = max(16, (rows * EARLY_NUM // EARLY_DEN) // 16 * 16)
    late = rows - early
    last = levels // 2
    halved = levels % 2 == 0
    rr = fv_ref.shape[0]

    def remote(src, dst, ssem, rsem, device):
        return pltpu.make_async_remote_copy(
            src_ref=src, dst_ref=dst, send_sem=ssem, recv_sem=rsem,
            device_id=device, device_id_type=pl.DeviceIdType.MESH,
        )

    barrier = pltpu.get_barrier_semaphore()
    for d in range(1, n):
        pl.semaphore_signal(
            barrier, inc=1, device_id={"fs": lax.rem(me + d, n)}, device_id_type=pl.DeviceIdType.MESH
        )
    for d in range(1, t):
        pl.semaphore_signal(
            barrier, inc=1, device_id={"tp": lax.rem(tp + d, t)}, device_id_type=pl.DeviceIdType.MESH
        )

    @pl.when(core == 0)
    def _():
        pltpu.make_async_copy(x_ref, xin, load_sem).start()
        pall[0, me] = pv_ref[...]

    @pl.when(core == 1)
    def _():
        pltpu.make_async_copy(oc_ref, xin, load_sem).start()
        pall[1, me] = po_ref[...]

    wall[me, :q] = wv_ref[...].astype(BF16)
    wall[me, q:] = wo_ref[...].astype(BF16)
    pl.semaphore_wait(barrier, n - 1 + t - 1)

    sends = []

    def go(copy):
        copy.start()
        sends.append(copy)
        return copy

    def to_all(buffer, target, ssem, rsem):
        out = []
        for d in range(1, n):
            peer = lax.rem(me + d, n)
            out.append(go(remote(buffer(peer), target, ssem.at[d], rsem.at[d], {"fs": peer})))
        return out

    def spread(place, ssem, rsem):
        own = place(me)
        first = [go(remote(own, own, ssem.at[0], rsem.at[0], {"fs": across}))]
        for d in range(1, levels):
            target = lax.rem(z + d, levels) * 2 + y
            first.append(go(remote(own, own, ssem.at[d], rsem.at[d], {"fs": target})))
        return first

    def pass_on(first, place, ssem, rsem):
        second = []
        for d in range(1, levels):
            first[d].wait_recv()
            block = place(lax.rem(z + levels - d, levels) * 2 + y)
            second.append(
                go(remote(block, block, ssem.at[levels + d], rsem.at[levels + d], {"fs": across}))
            )
        return first[:1] + second

    def edge(piece):
        return late if piece == CHUNKS else late * piece // CHUNKS // 16 * 16

    def span(piece, k, s):
        low, high = (edge(piece), edge(piece + 1)) if piece < CHUNKS else (late, rows)
        if halved and k == last:
            middle = low + (high - low) // 2 // 16 * 16
            low, high = (low, middle) if s == 0 else (middle, high)
        return low, high - low

    def at(level, column, low, size):
        return wall.at[level * 2 + column, pl.ds(low, size)]

    def ring(piece, k, s):
        low, size = span(piece, k, s)
        if size == 0:
            return None
        step = 1 if s == 0 else levels - 1
        level = lax.rem(z + (levels - step) * (k - 1), levels)
        column = y if piece <= CHUNKS else 1 - y
        place = at(level, column, low, size)
        target = lax.rem(z + step, levels) * 2 + y
        return go(remote(place, place, ring_send.at[s, k, piece], ring_recv.at[s, k, piece], {"fs": target}))

    def over(piece, k, s):
        low, size = span(piece, k, s)
        if size == 0:
            return None
        step = 1 if s == 0 else levels - 1
        level = lax.rem(z + (levels - step) * k, levels)
        place = at(level, y, low, size)
        return go(remote(place, place, y_send.at[s, k, piece], y_recv.at[s, k, piece], {"fs": across}))

    def landed(copy):
        if copy is not None:
            copy.wait_recv()

    proj_first = spread(lambda block: pall.at[core, block], p_send, p_recv)
    own_early = at(z, y, late, early)
    crossed = go(remote(own_early, own_early, y_send.at[1, 0, 0], y_recv.at[1, 0, 0], {"fs": across}))
    steps = {}
    for piece in range(CHUNKS + 1):
        for s in (0, 1):
            steps[piece, 1, s] = ring(piece, 1, s)
    proj_copies = pass_on(proj_first, lambda block: pall.at[core, block], p_send, p_recv)
    overs = [over(piece, 0, 0) for piece in range(CHUNKS)]

    for copy in proj_copies:
        copy.wait_recv()
    whole_proj = go(remote(pall.at[core], pall.at[core], core_send.at[0], core_recv.at[0], {"tp": partner}))
    pltpu.make_async_copy(x_ref, xin, load_sem).wait()
    pr[core] = jnp.dot(xin[...], flat(pall[core]), preferred_element_type=F32).astype(BF16)
    swapped = go(remote(pr.at[core], pr.at[core], core_send.at[1], core_recv.at[1], {"tp": partner}))
    swapped.wait_recv()
    for side, cot in ((0, vc_ref), (1, ret_ref)):
        grad = lax.dot_general(
            pr[side], cot[...], (((0,), (0,)), ((), ())), preferred_element_type=F32
        )
        for peer in range(n):
            gsend[peer, :, side * columns:(side + 1) * columns] = (
                grad[peer * rr:(peer + 1) * rr].astype(BF16)
            )
    grad_copies = to_all(lambda peer: gsend.at[peer], grecv.at[me], g_send, g_recv)

    crossed.wait_recv()
    for s in (0, 1):
        steps[CHUNKS + 1, 1, s] = ring(CHUNKS + 1, 1, s)

    for k in range(1, last + 1):
        for piece in range(CHUNKS + 2):
            if k == 1 and piece == CHUNKS + 1:
                for copy in grad_copies:
                    copy.wait_recv()
                total = gsend[me].astype(F32)
                for d in range(1, n):
                    total += grecv[lax.rem(me + d, n)].astype(F32)
                for side, refs in ((0, (fv_ref, sv_ref, nfv, nsv)), (1, (fo_ref, so_ref, nfo, nso))):
                    part = total[:, side * columns:(side + 1) * columns]
                    new_first, new_second, direction = adapt(refs[0][...], refs[1][...], part)
                    refs[2][...] = new_first
                    refs[3][...] = new_second
                    dall[me, :, side * columns:(side + 1) * columns] = direction
                dir_first = spread(lambda block: dall.at[block], d_send, d_recv)
            for s in (0, 1):
                landed(steps[piece, k, s])
                if k < last:
                    steps[piece, k + 1, s] = ring(piece, k + 1, s)
                if piece < CHUNKS:
                    overs.append(over(piece, k, s))

    for copy in pass_on(dir_first, lambda block: dall.at[block], d_send, d_recv):
        copy.wait_recv()
    sums = []
    for side in (0, 1):
        acc = jnp.zeros((rr, columns), F32)
        for k in range(n):
            acc += jnp.square(dall[k, :, side * columns:(side + 1) * columns].astype(F32))
        sums.append(jnp.sum(acc))
    line = lax.broadcasted_iota(jnp.int32, sq.shape[1:], 0)
    sq[tp] = jnp.where(line == 0, sums[0], sums[1])
    sq_copies = []
    for d in range(1, t):
        sq_copies.append(
            go(remote(sq.at[tp], sq.at[tp], q_send.at[d], q_recv.at[d], {"tp": lax.rem(tp + d, t)}))
        )
    for copy in sq_copies:
        copy.wait_recv()
    for copy in overs:
        landed(copy)
    whole_proj.wait_recv()
    for copy in sends:
        copy.wait_send()


def finish(q, count, sq_ref, wall_ref, pall_ref, own_v, own_o, dv_ref, do_ref, step_v, step_o, copy_v, copy_o):
    totals = jnp.sum(sq_ref[...], axis=0)
    scale_v = lax.rsqrt(totals[0:1, 0:1] / count + norm_eps)
    scale_o = lax.rsqrt(totals[1:2, 0:1] / count + norm_eps)
    n, _, lanes = wall_ref.shape
    dir_v, dir_o = dv_ref[...], do_ref[...]
    step_v[...] = jnp.dot(own_v[...], dir_v, preferred_element_type=F32) * scale_v
    step_o[...] = jnp.dot(own_o[...], dir_o, preferred_element_type=F32) * scale_o
    w_v = wall_ref[:, :q].astype(F32).reshape(n * q, lanes)
    w_o = wall_ref[:, q:].astype(F32).reshape(n * q, lanes)
    copy_v[...] = (
        w_v + jnp.dot(pall_ref[0], dir_v, preferred_element_type=F32) * scale_v
    ).astype(BF16)
    moved = w_o + jnp.dot(pall_ref[1], dir_o, preferred_element_type=F32) * scale_o
    copy_o[...] = moved.T.astype(BF16)


def per_device(
    n, t,
    inputs, value_cot, retained, output_cot, proj_value, proj_output, w_value, w_output,
    first_value, second_value, first_output, second_output,
):
    tokens, width = inputs.shape
    q, rank = proj_value.shape
    columns = value_cot.shape[1]
    rr = first_value.shape[0]
    last = n // 2 // 2
    vmem = pl.BlockSpec(memory_space=pltpu.VMEM)
    anywhere = pl.BlockSpec(memory_space=pl.ANY)
    dma = pltpu.SemaphoreType.DMA
    moment = jax.ShapeDtypeStruct((rr, columns), F32)
    wall, pall, dall, sq, first_v, second_v, first_o, second_o = pl.pallas_call(
        functools.partial(exchange, n, t),
        out_shape=(
            jax.ShapeDtypeStruct((n, 2 * q, columns), BF16),
            jax.ShapeDtypeStruct((2, n, q, rank), BF16),
            jax.ShapeDtypeStruct((n, rr, 2 * columns), BF16),
            jax.ShapeDtypeStruct((t, 8, 128), F32),
            moment, moment, moment, moment,
        ),
        in_specs=[anywhere, anywhere] + [vmem] * 10,
        out_specs=(vmem,) * 8,
        scratch_shapes=[
            pltpu.VMEM((tokens, width), BF16),
            pltpu.VMEM((2, tokens, rank), BF16),
            pltpu.VMEM((n, rr, 2 * columns), BF16),
            pltpu.VMEM((n, rr, 2 * columns), BF16),
            dma, dma((n,)), dma((n,)), dma((2,)), dma((2,)), dma((n,)), dma((n,)), dma((n,)), dma((n,)),
            dma((t,)), dma((t,)),
            dma((2, last + 1, CHUNKS + 2)), dma((2, last + 1, CHUNKS + 2)),
            dma((2, last + 1, CHUNKS)), dma((2, last + 1, CHUNKS)),
        ],
        compiler_params=pltpu.CompilerParams(
            collective_id=0, has_side_effects=True, vmem_limit_bytes=60 * 1024 * 1024
        ),
        name="exchange",
    )(
        inputs, output_cot, value_cot, retained, proj_value, proj_output, w_value, w_output.T,
        first_value, second_value, first_output, second_output,
    )
    lanes = 128
    tiles = columns // lanes
    dirs = dall.reshape(n * rr, 2 * columns)
    full = n * q
    step_v, step_o, copy_v, copy_o = pl.pallas_call(
        functools.partial(finish, q, float(rank * columns * t)),
        grid=(tiles,),
        out_shape=(
            jax.ShapeDtypeStruct((q, columns), F32),
            jax.ShapeDtypeStruct((q, columns), F32),
            jax.ShapeDtypeStruct((full, columns), BF16),
            jax.ShapeDtypeStruct((columns, full), BF16),
        ),
        in_specs=[
            pl.BlockSpec((t, 8, 128), lambda j: (0, 0, 0)),
            pl.BlockSpec((n, 2 * q, lanes), lambda j: (0, 0, j)),
            pl.BlockSpec((2, full, rank), lambda j: (0, 0, 0)),
            pl.BlockSpec((q, rank), lambda j: (0, 0)),
            pl.BlockSpec((q, rank), lambda j: (0, 0)),
            pl.BlockSpec((rank, lanes), lambda j: (0, j)),
            pl.BlockSpec((rank, lanes), lambda j: (0, j + tiles)),
        ],
        out_specs=(
            pl.BlockSpec((q, lanes), lambda j: (0, j)),
            pl.BlockSpec((q, lanes), lambda j: (0, j)),
            pl.BlockSpec((full, lanes), lambda j: (0, j)),
            pl.BlockSpec((lanes, full), lambda j: (j, 0)),
        ),
        compiler_params=pltpu.CompilerParams(vmem_limit_bytes=48 * 1024 * 1024),
        name="finish",
    )(sq, wall, pall.reshape(2, full, rank), proj_value, proj_output, dirs, dirs)
    return (step_v, step_o.T, copy_v, copy_o, first_v, second_v, first_o, second_o)


def solution(mesh):
    in_specs = (
        P("fs", None),
        P("fs", "tp"),
        P("fs", "tp"),
        P("fs", None),
        P("fs", None),
        P("fs", None),
        P("fs", "tp"),
        P("tp", "fs"),
        P("fs", "tp"),
        P("fs", "tp"),
        P("fs", "tp"),
        P("fs", "tp"),
    )
    out_specs = (
        P("fs", "tp"),
        P("tp", "fs"),
        P(None, "tp"),
        P("tp", None),
        P("fs", "tp"),
        P("fs", "tp"),
        P("fs", "tp"),
        P("fs", "tp"),
    )
    return jax.shard_map(
        functools.partial(per_device, mesh.shape["fs"], mesh.shape["tp"]),
        mesh=mesh, in_specs=in_specs, out_specs=out_specs, check_vma=False,
    )
```
